256 devices in a mesh: sp: 64 (over z, y, core), tp: 4 (over x).
Axes of the slice: x: 4, y: 4, z: 8, core: 2. Of those that a mesh axis runs over, the one named last changes fastest.
Arguments:
- conv_outer: bfloat16 [49152, 2048], P('sp', 'tp'), may hold values from -6 to 6
- conv_inner: bfloat16 [49152, 2048], P('sp', 'tp'), may hold values from -6 to 6
- conv_input: bfloat16 [49152, 2048], P('sp', 'tp'), may hold values from -6 to 6
- conv_taps: float32 [3, 2048], P(None, 'tp'), may hold values from -3.5 to 3.5
- out_weight: bfloat16 [2048, 2048], P('tp'), may hold values from -0.125 to 0.125
- mix_gate: bfloat16 [49152, 2048], P(('sp', 'tp')), may hold values from -8 to 8
- residual: bfloat16 [49152, 2048], P(('sp', 'tp')), may hold values from -6 to 6
- mix_gain: float32 [2048], replicated, may hold values from 0.1 to 1.9
- expert_gain: float32 [2048], replicated, may hold values from 0.1 to 1.9
- expert_ids: int32 [49152, 2], P(('sp', 'tp')), may hold values from 0 to 63, all different within a row; in each aligned block of 192 rows (0 to 191, 192 to 383, ...) at most 12 rows name the same one
- group_share: float32 [49152], P(('sp', 'tp')), may hold values from 0.25 to 1
- pair_scores: float32 [49152, 2], P(('sp', 'tp')), may hold values from -8 to 8
- gate_experts: bfloat16 [64, 2048, 512], P('sp'), may hold values from -0.125 to 0.125
- up_experts: bfloat16 [64, 2048, 512], P('sp'), may hold values from -0.125 to 0.125
- down_experts: bfloat16 [64, 512, 2048], P('sp'), may hold values from -0.25 to 0.25
Outputs:
- layer_out: bfloat16 [49152, 2048], P(('sp', 'tp'))
The draws below stay inside these ranges and needn't reach their ends.
Inputs may be any that keep to these rules, and one draw needn't show every extreme that they name: `expert_ids`: within the rows of one device (aligned blocks of 192 rows), no expert is named by more than 12 rows, a bound that some block reaches; the 2 experts of a row differ.
All inputs are finite; a program needn't handle non-finite values.
Results may differ from the reference program's by a relative error of at most 0.0069.
Values may be sent and summed in bfloat16 or wider, within the bound.
No kernel may reach another device: no remote copies, remote signals or barrier semaphores. Data moves between devices by JAX's collectives and lax.ppermute only.
A program may use at most 128 MiB of HBM per device.

```python
import math
import jax
import jax.numpy as jnp
import numpy as np
from jax import lax

D = 2048
CW = 2048
FF = 512
KSIZE = 3
TOP = 2
TOK_DEV = 192
EXPERTS = 64
CAP = 12
TOKENS = 49152


def block_scale(stream_key, dims, cuts, smallest, largest):
    loudness, own = 1.0, jax.random.fold_in(stream_key, 6)
    for axis_at, blocks in cuts:
        steps = jnp.exp(jax.random.uniform(jax.random.fold_in(own, axis_at), (blocks,), jnp.float32, smallest / len(cuts), largest / len(cuts)))
        loudness = loudness * jnp.repeat(steps, dims[axis_at] // blocks).reshape([-1 if axis == axis_at else 1 for axis in range(len(dims))])
    return loudness


def routed_block(own_key, own, number, rows, amount, top, limit, skew):
    order = jax.random.permutation(own_key, amount)
    packed, ordinary = load_shares(amount, rows * top, limit, skew, True), load_shares(amount, rows * top, limit, skew, False)
    places = jnp.arange(amount)

    def named(sizes, rotation):
        used = int((sizes > 0).sum())
        fixed = max(1, used // 4)
        moved = fixed + (places - fixed + rotation * (used - fixed)) % max(1, amount - fixed)
        return jnp.zeros((amount,), jnp.int32).at[order[jnp.where(places < fixed, places, moved)]].set(jnp.asarray(sizes, jnp.int32))

    sizes = jnp.where(number % 4 == 0, named(packed, number // 4), named(ordinary, number - number // 4 - 1))
    mixed = jax.random.permutation(jax.random.fold_in(own, 3), amount)
    donor, sink = mixed[0:amount // 2 * 2:2], mixed[1:amount // 2 * 2:2]
    margin = jnp.minimum(sizes[donor] - 1, limit - sizes[sink]) // 2
    margin = jnp.where((donor == order[0]) | (sink == order[0]) | (sizes[sink] == 0), 0, jnp.maximum(margin, 0))
    moved = jax.random.randint(jax.random.fold_in(own, 4), (amount // 2,), 0, 1 << 20) % (margin + 1)
    sizes = sizes.at[donor].add(-moved).at[sink].add(moved)
    members = jnp.searchsorted(jnp.cumsum(sizes), jnp.arange(rows * top), side="right").astype(jnp.int32)
    table = members.reshape(top, rows).T
    table = table[jax.random.permutation(jax.random.fold_in(own, 1), rows)]
    rotation = jax.random.randint(jax.random.fold_in(own, 2), (rows, 1), 0, top)
    return jnp.take_along_axis(table, (jnp.arange(top)[None, :] + rotation) % top, axis=1)


def load_shares(number_of, total, reach, slope, full):
    portions = [(1 << 20) // math.isqrt(standing ** slope) + 1 for standing in range(1, number_of + 1)]
    largest = reach if full else min(reach, max(-(-total // number_of), total * portions[0] // sum(portions)))
    least = 1 if total - largest >= number_of - 1 else 0
    given, spare = [largest] + [least] * (number_of - 1), total - largest - least * (number_of - 1)
    while spare > 0:
        candidates = [i for i in range(1, number_of) if given[i] < largest] or [i for i in range(1, number_of) if given[i] < reach]
        mass, budget = sum([portions[i] for i in candidates]), spare
        for i in candidates:
            extra = min(reach - given[i], max(1, budget * portions[i] // mass), spare)
            given[i] = given[i] + extra
            spare = spare - extra
    return np.array(given)


def bell_draw(rng, extent, spread, limit, pieces=(), kind=jnp.bfloat16):
    level = block_scale(rng, extent, pieces, -0.22, 0.18) if pieces else 1.0
    values = jax.random.normal(rng, extent, jnp.float32) * spread * level
    return jnp.minimum(jnp.maximum(values, -limit), limit).astype(kind)


def setup_inputs(seed: int = 0) -> dict:
    key_list = jax.random.split(jax.random.key(seed), 16)
    conv_outer = bell_draw(key_list[0], (TOKENS, CW), 1.0, 6.0, ((0, 64), (1, 4)))
    conv_inner = bell_draw(key_list[1], (TOKENS, CW), 1.0, 6.0, ((0, 64), (1, 4)))
    conv_input = bell_draw(key_list[2], (TOKENS, CW), 1.0, 6.0, ((0, 64), (1, 4)))
    conv_taps = bell_draw(key_list[3], (KSIZE, CW), KSIZE ** -0.5, 3.5, ((1, 4),), jnp.float32)
    out_weight = bell_draw(key_list[4], (CW, D), CW ** -0.5, 0.125, ((0, 4),))
    mix_gate = bell_draw(key_list[5], (TOKENS, D), 1.5, 8.0, ((0, 256),))
    residual = bell_draw(key_list[6], (TOKENS, D), 1.0, 6.0, ((0, 256),))
    mix_gain = jnp.clip(1.0 + 0.18 * jax.random.normal(key_list[7], (D,), jnp.float32), 0.1, 1.9)
    expert_gain = jnp.clip(1.0 + 0.18 * jax.random.normal(key_list[8], (D,), jnp.float32), 0.1, 1.9)
    expert_ids_keys = jax.random.split(jax.random.fold_in(key_list[9], 1), TOKENS // TOK_DEV)
    expert_ids_turns = jax.random.permutation(jax.random.fold_in(key_list[9], 3), TOKENS // TOK_DEV)
    expert_ids = jax.vmap(lambda own, number: routed_block(jax.random.fold_in(key_list[9], 2), own, number, TOK_DEV, EXPERTS, TOP, CAP, 1))(expert_ids_keys, expert_ids_turns).reshape((TOKENS, TOP))
    group_share = jnp.clip(0.25 + 0.75 * jax.random.uniform(key_list[10], (TOKENS,), jnp.float32) ** block_scale(key_list[10], (TOKENS,), ((0, 256),), -0.2, 0.2), 0.25, 1.0)
    pair_scores = bell_draw(key_list[11], (TOKENS, TOP), 1.5, 8.0, ((0, 256),), jnp.float32)
    gate_experts = bell_draw(key_list[12], (EXPERTS, D, FF), D ** -0.5, 0.125, ((0, 64),))
    up_experts = bell_draw(key_list[13], (EXPERTS, D, FF), D ** -0.5, 0.125, ((0, 64),))
    down_experts = bell_draw(key_list[14], (EXPERTS, FF, D), FF ** -0.5, 0.25, ((0, 64),))
    return {"conv_outer": conv_outer, "conv_inner": conv_inner, "conv_input": conv_input, "conv_taps": conv_taps, "out_weight": out_weight, "mix_gate": mix_gate, "residual": residual, "mix_gain": mix_gain, "expert_gain": expert_gain, "expert_ids": expert_ids, "group_share": group_share, "pair_scores": pair_scores, "gate_experts": gate_experts, "up_experts": up_experts, "down_experts": down_experts}


epsilon = 1e-06

def rms_scale(values, gain):
    return values * lax.rsqrt(lax.optimization_barrier(jnp.mean(values * values, axis=-1, keepdims=True)) + epsilon) * gain

def reference(conv_outer, conv_inner, conv_input, conv_taps, out_weight, mix_gate, residual, mix_gain, expert_gain, expert_ids, group_share, pair_scores, gate_experts, up_experts, down_experts):
    inner = conv_inner.astype(jnp.float32) * conv_input.astype(jnp.float32)
    length = inner.shape[0]
    padded = jnp.pad(inner, ((KSIZE - 1, 0), (0, 0)))
    conv = conv_taps[0] * padded[0:length]
    for offset in range(1, KSIZE):
        conv = conv + conv_taps[offset] * padded[offset:offset + length]
    mixed_rows = (conv_outer.astype(jnp.float32) * conv).astype(jnp.bfloat16)
    projected = jnp.dot(mixed_rows, out_weight, preferred_element_type=jnp.float32)
    mixed = jax.nn.sigmoid(mix_gate.astype(jnp.float32)) * projected
    hidden_state = (residual.astype(jnp.float32) + rms_scale(mixed, mix_gain)).astype(jnp.bfloat16)
    normed = rms_scale(hidden_state.astype(jnp.float32), expert_gain).astype(jnp.bfloat16)
    flat_ids = expert_ids.reshape(-1).astype(jnp.int32)
    total = flat_ids.shape[0]
    bound = TOKENS // TOK_DEV * CAP

    def one_expert(carried, expert):
        chosen = jnp.nonzero(flat_ids == expert, size=bound, fill_value=total)[0].astype(jnp.int32)
        rows = normed[jnp.minimum(chosen, total - 1) // TOP]
        first = jnp.dot(rows, gate_experts[expert], preferred_element_type=jnp.float32)
        second = jnp.dot(rows, up_experts[expert], preferred_element_type=jnp.float32)
        inner_hidden = (jax.nn.silu(first) * second).astype(jnp.bfloat16)
        result = jnp.dot(inner_hidden, down_experts[expert], preferred_element_type=jnp.float32).astype(jnp.bfloat16)
        return (carried.at[chosen].set(result, mode='drop'), None)
    start = jnp.zeros((total, D), jnp.bfloat16)
    assigned, unused = lax.scan(one_expert, start, jnp.arange(EXPERTS, dtype=jnp.int32))
    assigned = assigned.reshape(TOKENS, TOP, D)
    weights = group_share[:, None] * jax.nn.softmax(pair_scores, axis=-1)
    result = hidden_state.astype(jnp.float32)
    for slot in range(TOP):
        result = result + weights[:, slot:slot + 1] * assigned[:, slot].astype(jnp.float32)
    return result.astype(jnp.bfloat16)
```

```python
import functools

import jax
import jax.numpy as jnp
from jax import lax
from jax.experimental import pallas as pl
from jax.experimental.pallas import tpu as pltpu
from jax.sharding import Mesh
from jax.sharding import PartitionSpec as P

SP = ("sp_0", "sp_1", "sp_2")
SP_TP = ("sp_0", "sp_1", "sp_2", "tp")


epsilon = 1e-06
SLOTS = ((0, 12),)


def passed_along(value, axis, steps):
    count = lax.axis_size(axis)
    leading, last = (max(0, -steps), min(count, count - steps))
    return lax.ppermute(value, axis, [(source, source + steps) for source in range(leading, last)])


def turned(value, axis, steps):
    count = lax.axis_size(axis)
    if steps % count == 0:
        return value
    return lax.ppermute(value, axis, [(source, (source + steps) % count) for source in range(count)])


def split_up(value, dim, peers):
    before, after = (value.shape[:dim], value.shape[dim + 1 :])
    return jnp.moveaxis(value.reshape(*before, peers, -1, *after), dim, 0)


def sent_and_summed(value, axis, dim):
    peers = lax.axis_size(axis)
    parts = lax.all_to_all(split_up(value, dim, peers), axis, 0, 0, tiled=True)
    return jnp.sum(parts.astype(jnp.float32), axis=0)


def rms_scale(values, gain):
    return values * lax.rsqrt(jnp.mean(values * values, axis=-1, keepdims=True) + epsilon) * gain


def experts_kernel(group, x, *refs):
    weights, out, hidden = refs[:6], refs[6], refs[7]
    step = pl.program_id(0)
    units = weights[0].shape[2]
    for k in range(2):

        @pl.when(step == k)
        def _(k=k):
            gate, up = weights[3 * k], weights[3 * k + 1]
            rows = x[...]
            first = jnp.dot(rows, gate[0], preferred_element_type=jnp.float32)
            second = jnp.dot(rows, up[0], preferred_element_type=jnp.float32)
            value = first / (1.0 + jnp.exp(-first)) * second
            which = lax.broadcasted_iota(jnp.int32, (rows.shape[0], 1), 0) // group % 2
            hidden[:, k * units : (k + 1) * units] = jnp.where(which == k, value, 0.0).astype(
                jnp.bfloat16
            )

    @pl.when(step == 2)
    def _():
        down, other = weights[2], weights[5]
        total = jnp.dot(hidden[:, :units], down[0], preferred_element_type=jnp.float32)
        total += jnp.dot(hidden[:, units:], other[0], preferred_element_type=jnp.float32)
        out[...] = total.astype(out.dtype)


def experts_of_chip(rows, weights, group):
    units, wide = weights[2].shape[1:]
    count = rows.shape[0]
    whole = pl.BlockSpec(rows.shape, lambda s: (0, 0))
    return pl.pallas_call(
        functools.partial(experts_kernel, group),
        grid=(3,),
        in_specs=[whole] + [pl.BlockSpec(w.shape, lambda s: (0, 0, 0)) for w in weights],
        out_specs=whole,
        out_shape=jax.ShapeDtypeStruct(rows.shape, rows.dtype),
        scratch_shapes=[pltpu.VMEM((count, 2 * units), jnp.bfloat16)],
        cost_estimate=pl.CostEstimate(
            flops=12 * count * wide * units,
            bytes_accessed=12 * wide * units + 4 * count * wide,
            transcendentals=2 * count * units,
        ),
        name="experts",
    )(rows, *weights)


def combine_kernel(count, base, *refs):
    highs, lows, blocks, out = refs[:count], refs[count : 2 * count], refs[2 * count : -1], refs[-1]
    total = base[...].astype(jnp.float32)
    for high, low, block in zip(highs, lows, blocks):
        rows = block[...]
        total += jnp.dot(high[...], rows, preferred_element_type=jnp.float32)
        total += jnp.dot(low[...], rows, preferred_element_type=jnp.float32)
    out[...] = total.astype(out.dtype)


def combined(base, highs, lows, blocks, dtype):
    rows, wide = base.shape
    part = 512
    columns = lambda n: pl.BlockSpec((n, part), lambda j: (0, j))
    spreads = [pl.BlockSpec(h.shape, lambda j: (0, 0)) for h in highs]
    return pl.pallas_call(
        functools.partial(combine_kernel, len(blocks)),
        grid=(wide // part,),
        in_specs=[columns(rows)] + spreads + spreads + [columns(b.shape[0]) for b in blocks],
        out_specs=columns(rows),
        out_shape=jax.ShapeDtypeStruct(base.shape, dtype),
        cost_estimate=pl.CostEstimate(
            flops=4 * rows * wide * sum(b.shape[0] for b in blocks),
            bytes_accessed=8 * rows * wide,
            transcendentals=0,
        ),
        name="combine",
    )(base, *highs, *lows, *blocks)


def per_device(
    conv_outer,
    conv_inner,
    conv_input,
    conv_taps,
    out_weight,
    mix_gate,
    residual,
    mix_gain,
    expert_gain,
    expert_ids,
    group_share,
    pair_scores,
    gate_experts,
    up_experts,
    down_experts,
):
    planes, lanes, cores = (lax.axis_size(a) for a in SP)
    weights_own = [gate_experts, up_experts, down_experts]
    experts = weights_own + [turned(w, "sp_2", 1) for w in weights_own]

    kept = conv_taps.shape[0] - 1
    earlier = passed_along((conv_inner[-kept:], conv_input[-kept:]), SP, 1)
    inner = jnp.concatenate(
        [
            earlier[0].astype(jnp.float32) * earlier[1].astype(jnp.float32),
            conv_inner.astype(jnp.float32) * conv_input.astype(jnp.float32),
        ],
        0,
    )
    length = conv_inner.shape[0]
    conv = conv_taps[0] * inner[0:length]
    for offset in range(1, kept + 1):
        conv = conv + conv_taps[offset] * inner[offset : offset + length]
    mixed_rows = (conv_outer.astype(jnp.float32) * conv).astype(jnp.bfloat16)
    own_rows = residual.shape[0]
    projected = sent_and_summed(
        jnp.dot(mixed_rows, out_weight, preferred_element_type=jnp.float32).astype(jnp.bfloat16),
        "tp",
        0,
    )
    mixed = jax.nn.sigmoid(mix_gate.astype(jnp.float32)) * projected
    hidden_state = (residual.astype(jnp.float32) + rms_scale(mixed, mix_gain)).astype(jnp.bfloat16)
    normed = rms_scale(hidden_state.astype(jnp.float32), expert_gain).astype(jnp.bfloat16)

    experts_all = planes * lanes * cores
    per_token = expert_ids.shape[1]
    c = lax.axis_index("sp_2")
    chips = planes * lanes
    relative = expert_ids // cores * cores + (expert_ids - c) % cores
    flat = relative.reshape(-1)
    onehot = (flat[:, None] == jnp.arange(experts_all, dtype=jnp.int32)[None, :]).astype(jnp.int32)
    ranks = jnp.sum((jnp.cumsum(onehot, axis=0) - 1) * onehot, axis=1)
    expert_of, rank_of = relative, ranks.reshape(own_rows, per_token)
    weights = group_share[:, None] * jax.nn.softmax(pair_scores, axis=-1)

    parts = []
    highs, lows, blocks = [], [], []
    for start, stop in SLOTS:
        group = stop - start
        slots = jnp.arange(experts_all * group, dtype=jnp.int32)
        inside = (rank_of >= start) & (rank_of < stop)
        slot_of = jnp.where(inside, expert_of * group + rank_of - start, -1)
        turned_slots = slot_of.T
        pick = sum(
            (slots[:, None] == turned_slots[k][None, :]).astype(jnp.bfloat16)
            for k in range(per_token)
        )
        spread = sum(
            jnp.where(slot_of[:, k : k + 1] == slots[None, :], weights[:, k : k + 1], 0.0)
            for k in range(per_token)
        )
        high = spread.astype(jnp.bfloat16)
        highs.append(high)
        lows.append((spread - high.astype(jnp.float32)).astype(jnp.bfloat16))
        rows = jnp.dot(pick, normed, preferred_element_type=jnp.float32).astype(jnp.bfloat16)
        rows = rows.reshape(chips, cores * group, -1)
        arrived = lax.all_to_all(rows, ("sp_0", "sp_1"), 0, 0, tiled=True)
        parts.append((group, arrived))
    for group, arrived in parts:
        served = experts_of_chip(arrived.reshape(-1, arrived.shape[2]), experts, group)
        back = lax.all_to_all(
            served.reshape(arrived.shape), ("sp_0", "sp_1"), 0, 0, tiled=True
        )
        blocks.append(back.reshape(-1, arrived.shape[2]))
    return combined(hidden_state, highs, lows, blocks, jnp.bfloat16)


def solution(mesh):
    torus = Mesh(mesh.devices.reshape(8, 4, 2, mesh.shape["tp"]), ("sp_0", "sp_1", "sp_2", "tp"))
    return jax.shard_map(
        per_device,
        mesh=torus,
        in_specs=(
            P(SP, "tp"),
            P(SP, "tp"),
            P(SP, "tp"),
            P(None, "tp"),
            P("tp", None),
            P(SP_TP, None),
            P(SP_TP, None),
            P(),
            P(),
            P(SP_TP, None),
            P(SP_TP),
            P(SP_TP, None),
            P(SP, None, None),
            P(SP, None, None),
            P(SP, None, None),
        ),
        out_specs=P(SP_TP, None),
        check_vma=False,
    )
```
